32 devices in a mesh: grp: 2 (over y), ep: 4 (over z), tp: 4 (over x, core).
Axes of the slice: x: 2, y: 2, z: 4, core: 2. Of those that a mesh axis runs over, the one named last changes fastest.
Arguments:
- queries: bfloat16 [4096, 768], P(('grp', 'ep'), 'tp'), parts along dimension 0, may hold values from -6 to 6
- key_value: bfloat16 [4096, 4, 128], P(('grp', 'ep'), 'tp'), parts along dimension 0, may hold values from -6 to 6
- key_bias: bfloat16 [4, 4096], P('tp', ('grp', 'ep')), parts along dimension 1, may hold values from -20 to 0
- out_weight: bfloat16 [768, 2048], P('tp'), may hold values from -0.75 to 0.75
- expert_input: bfloat16 [4096, 2048], P(('grp', 'ep', 'tp')), parts along dimension 0, may hold values from -6 to 6
- norm_gain: float32 [2048], replicated, may hold values from 0.1 to 1.9
- routes: int32 [4096, 4], P(('grp', 'ep', 'tp')), parts along dimension 0, may hold values from 0 to 15, as said below
- route_weights: float32 [4096, 4], P(('grp', 'ep', 'tp')), parts along dimension 0, may hold values from 0.2 to 1
- gate_weight: bfloat16 [16, 2048, 512], P(('ep', 'tp')), may hold values from -0.125 to 0.125
- up_weight: bfloat16 [16, 2048, 512], P(('ep', 'tp')), may hold values from -0.125 to 0.125
- down_weight: bfloat16 [16, 512, 2048], P(('ep', 'tp')), may hold values from -0.25 to 0.25
- shared_gate: bfloat16 [2048, 256], replicated, may hold values from -0.125 to 0.125
- shared_up: bfloat16 [2048, 256], replicated, may hold values from -0.125 to 0.125
- shared_down: bfloat16 [256, 2048], replicated, may hold values from -0.375 to 0.375
Outputs:
- mixer_output: bfloat16 [4096, 2048], P(('grp', 'ep', 'tp')), parts along dimension 0
- expert_output: bfloat16 [4096, 2048], P(('grp', 'ep', 'tp')), parts along dimension 0
The draws below stay inside these ranges and needn't reach their ends.
There are 2 independent parts, one for each index of `grp`. The reference program is written for one: setup_inputs(seed, part) draws one part's arguments, and reference() takes and returns one part's arrays. A program takes and returns all parts, laid end to end along the dimension named above; an argument that names none is the same for every part. Nothing has to cross between parts.
Inputs may be any that keep to these rules, and one draw needn't show every extreme that they name: `routes`: each row names 4 different experts. Among the 128 rows of one device no expert is named more than 48 times, and in every draw one expert is named exactly 48 times in the rows of every device.
All inputs are finite; a program needn't handle non-finite values.
Results may differ from the reference program's by a relative error of at most 0.009.
Values may be sent and summed in bfloat16 or wider, within the bound.
No kernel may reach another device: no remote copies, remote signals or barrier semaphores. Data moves between devices by JAX's collectives and lax.ppermute only.
A program may use at most 128 MiB of HBM per device.

```python
import math
import jax
import jax.numpy as jnp
import numpy as np
from jax import lax

D = 2048
HD = 64
HEADS = 12
KEY_HEAD_COUNT = 4
EFF = 512
SFF = 256
TOPK = 4
TOK = 128
SPAN = 512
DEVSEQ = 4
SEQUENCE_LENGTH = 2048
TOTAL_POSITIONS = 2048
TOKENS = 2048
EXPERTS = 16
CAP = 48
HOT = 2
N_TP = 4


def draw_routes(key, part):
    key_hot = jax.random.fold_in(key, 11)
    key_order = jax.random.fold_in(key, 12)
    key_rows = jax.random.fold_in(key, 13)
    sources = TOKENS // TOK
    hot_expert = jax.random.randint(key_hot, (), 0, EXPERTS, dtype=jnp.int32)
    ordinal = jnp.broadcast_to(jnp.arange(EXPERTS, dtype=jnp.int32), (sources, EXPERTS))
    orders = jax.random.permutation(key_order, ordinal, axis=1, independent=True)
    hot_place = jnp.argmax(orders == hot_expert, axis=1)
    columns = jnp.arange(EXPERTS, dtype=jnp.int32)[None, :]
    leading = orders[:, :1]
    orders = jnp.where(columns == 0, hot_expert, jnp.where(columns == hot_place[:, None], leading, orders))
    remaining = TOK * TOPK - HOT * CAP
    others = EXPERTS - HOT
    counts = np.array([CAP] * HOT + [remaining // others + (1 if index < remaining % others else 0) for index in range(others)])
    rank_list = np.repeat(np.arange(EXPERTS), counts)
    tickets = orders[:, rank_list]
    laid_out = jnp.transpose(tickets.reshape(sources, TOPK, TOK), (0, 2, 1))
    row_ordinal = jnp.broadcast_to(jnp.arange(TOK, dtype=jnp.int32), (sources, TOK))
    row_orders = jax.random.permutation(key_rows, row_ordinal, axis=1, independent=True)
    shuffled = jnp.take_along_axis(laid_out, jnp.broadcast_to(row_orders[:, :, None], laid_out.shape), axis=1)
    return shuffled.reshape(TOKENS, TOPK).astype(jnp.int32)


def draw_key_bias(key, part):
    ranking = jax.random.permutation(jax.random.fold_in(key, 21), KEY_HEAD_COUNT)
    fast_count = KEY_HEAD_COUNT // 2
    is_fast = ranking < fast_count
    drawn_version = jnp.where(is_fast, -jnp.log(40.0), -jnp.log(float(SEQUENCE_LENGTH)) - 1.0)[:, None]
    jaggedness = jax.random.uniform(jax.random.fold_in(key, 22), (KEY_HEAD_COUNT, TOTAL_POSITIONS), jnp.float32, -0.5, 0.5)
    block_by_block = jax.random.uniform(jax.random.fold_in(key, 23), (KEY_HEAD_COUNT, TOTAL_POSITIONS // SPAN), jnp.float32, -0.7, 0.7)
    block_by_block = jnp.repeat(block_by_block, SPAN, axis=1)
    spike_events = jax.random.randint(jax.random.fold_in(key, 24), (KEY_HEAD_COUNT, TOTAL_POSITIONS), 0, SEQUENCE_LENGTH) < 3
    spike_height = jax.random.uniform(jax.random.fold_in(key, 25), (KEY_HEAD_COUNT, TOTAL_POSITIONS), jnp.float32, -1.2, -0.3)
    return jnp.where(spike_events, spike_height, drawn_version + jaggedness + block_by_block).astype(jnp.bfloat16)


def level_of(stream_key, extent, split, smallest, high):
    gain, own = 1.0, jax.random.fold_in(stream_key, 6)
    for dim, blocks in split:
        heights = jnp.exp(jax.random.uniform(jax.random.fold_in(own, dim), (blocks,), jnp.float32, smallest / len(split), high / len(split)))
        gain = gain * jnp.repeat(heights, extent[dim] // blocks).reshape([-1 if axis == dim else 1 for axis in range(len(extent))])
    return gain


def gaussian(key, shape, spread, limit, shards=(), kind=jnp.bfloat16):
    drawn = spread * jax.random.normal(key, shape, jnp.float32)
    if shards:
        drawn = drawn * level_of(key, shape, shards, -0.22, 0.18)
    return jnp.clip(drawn, -limit, limit).astype(kind)


def setup_inputs(seed: int = 0, part: int = 0) -> dict:
    keys = jax.random.split(jax.random.key(seed), 15)
    part_splits = jax.random.split(jax.random.fold_in(keys[14], part), 15)
    return {
        "queries": gaussian(part_splits[0], (TOTAL_POSITIONS, HEADS * HD), 1.0, 6.0, ((0, 4), (1, 4))),
        "key_value": gaussian(part_splits[1], (TOTAL_POSITIONS, KEY_HEAD_COUNT, 2 * HD), 1.0, 6.0, ((0, 4), (1, 4))),
        "key_bias": draw_key_bias(jax.random.fold_in(jax.random.fold_in(keys[14], part), 71), part),
        "out_weight": gaussian(keys[3], (HEADS * HD, D), HD ** -0.5, 0.75, ((0, 4),)),
        "expert_input": gaussian(part_splits[4], (TOKENS, D), 1.0, 6.0, ((0, 16),)),
        "norm_gain": jnp.clip(1.0 + 0.18 * jax.random.normal(keys[5], (D,), jnp.float32), 0.1, 1.9),
        "routes": draw_routes(jax.random.fold_in(jax.random.fold_in(keys[14], part), 71), part),
        "route_weights": jnp.clip(jnp.exp(math.log(1.0) - 1.609438 * jax.random.uniform(part_splits[7], (TOKENS, TOPK), jnp.float32) ** level_of(part_splits[7], (TOKENS, TOPK), ((0, 16),), -0.2, 0.2)), 0.2, 1.0),
        "gate_weight": gaussian(keys[8], (EXPERTS, D, EFF), D ** -0.5, 0.125, ((0, 16),)),
        "up_weight": gaussian(keys[9], (EXPERTS, D, EFF), D ** -0.5, 0.125, ((0, 16),)),
        "down_weight": gaussian(keys[10], (EXPERTS, EFF, D), EFF ** -0.5, 0.25, ((0, 16),)),
        "shared_gate": gaussian(keys[11], (D, SFF), D ** -0.5, 0.125),
        "shared_up": gaussian(keys[12], (D, SFF), D ** -0.5, 0.125),
        "shared_down": gaussian(keys[13], (SFF, D), SFF ** -0.5, 0.375),
    }


def piece_update(running, query_rows, key_rows, value_rows, key_offset, allowed):
    totals, kept_sum = running
    logits = jnp.einsum('sgrd,kgd->grsk', query_rows.astype(jnp.float32), key_rows.astype(jnp.float32)) * 0.125
    logits = logits + key_offset.astype(jnp.float32)[:, None, None, :]
    log_keep = jnp.where(allowed, -jax.nn.softplus(logits), 0.0)
    log_after = lax.cumsum(log_keep, axis=3, reverse=True) - log_keep
    weights = jnp.where(allowed, jnp.exp(jax.nn.log_sigmoid(logits) + log_after + kept_sum[..., None]), 0.0)
    weights = weights.astype(jnp.bfloat16)
    totals = totals + jnp.einsum('grsk,kgd->grsd', weights.astype(jnp.float32), value_rows.astype(jnp.float32))
    return (totals, kept_sum + lax.optimization_barrier(jnp.sum(log_keep, axis=3)))

def mixer_reference(queries, key_value, key_bias, out_weight):
    per_group = HEADS // KEY_HEAD_COUNT
    block_count = TOTAL_POSITIONS // SPAN
    query_blocks = queries.reshape(block_count, SPAN, KEY_HEAD_COUNT, per_group, HD)
    key_blocks = key_value[..., :HD].reshape(block_count, SPAN, KEY_HEAD_COUNT, HD)
    value_blocks = key_value[..., HD:].reshape(block_count, SPAN, KEY_HEAD_COUNT, HD)
    bias_blocks = jnp.transpose(key_bias.reshape(KEY_HEAD_COUNT, block_count, SPAN), (1, 0, 2))
    positions = jnp.arange(SPAN, dtype=jnp.int32)
    strict_mask = positions[None, :] < positions[:, None]
    full_mask = jnp.ones((SPAN, SPAN), dtype=bool)

    def one_block(block_index):
        query_rows = query_blocks[block_index]
        initial = (jnp.zeros((KEY_HEAD_COUNT, per_group, SPAN, HD), jnp.float32), jnp.zeros((KEY_HEAD_COUNT, per_group, SPAN), jnp.float32))
        running = piece_update(initial, query_rows, key_blocks[block_index], value_blocks[block_index], bias_blocks[block_index], strict_mask)

        def advance(distance, current):
            source = block_index - distance
            return piece_update(current, query_rows, key_blocks[source], value_blocks[source], bias_blocks[source], full_mask)
        chain_place = jnp.minimum((block_index + 2) % DEVSEQ, block_index)
        running = lax.fori_loop(1, chain_place + 1, advance, running)
        return running[0].astype(jnp.bfloat16)
    attended = lax.map(one_block, jnp.arange(block_count, dtype=jnp.int32))
    weight_blocks = out_weight.reshape(KEY_HEAD_COUNT, per_group, HD, D)
    group_heads = KEY_HEAD_COUNT // N_TP
    summed = jnp.zeros((block_count, SPAN, D), jnp.float32)
    for group_index in range(N_TP):
        part_rows = attended[:, group_index * group_heads:(group_index + 1) * group_heads].astype(jnp.float32)
        part_weight = weight_blocks[group_index * group_heads:(group_index + 1) * group_heads].astype(jnp.float32)
        group_terms = jnp.einsum('bgrsd,grde->bse', part_rows, part_weight).astype(jnp.bfloat16)
        summed = summed + group_terms.astype(jnp.float32)
    return summed.reshape(TOTAL_POSITIONS, D).astype(jnp.bfloat16)

def experts_reference(expert_input, norm_gain, routes, route_weights, gate_weight, up_weight, down_weight, shared_gate, shared_up, shared_down):
    widened = expert_input.astype(jnp.float32)
    normed = (widened * lax.rsqrt(lax.optimization_barrier(jnp.mean(widened * widened, axis=-1, keepdims=True)) + 1e-06) * norm_gain).astype(jnp.bfloat16)
    sources = TOKENS // TOK
    pair_count = TOK * TOPK
    block_routes = routes.reshape(sources, pair_count)
    one_hot = (block_routes[..., None] == jnp.arange(EXPERTS, dtype=jnp.int32)).astype(jnp.int32)
    slot_index = lax.optimization_barrier(jnp.sum((jnp.cumsum(one_hot, axis=1) - one_hot) * one_hot, axis=2))
    placing = (block_routes * sources + jnp.arange(sources, dtype=jnp.int32)[:, None]) * CAP + slot_index
    empty_pair = TOKENS * TOPK
    table = jnp.full((EXPERTS * sources * CAP,), empty_pair, jnp.int32)
    table = table.at[placing.reshape(-1)].set(jnp.arange(empty_pair, dtype=jnp.int32))
    table = table.reshape(EXPERTS, sources * CAP)
    padded_rows = jnp.concatenate([normed, jnp.zeros((1, D), jnp.bfloat16)], axis=0)
    padded_weights = jnp.concatenate([route_weights.reshape(-1), jnp.zeros((1,), jnp.float32)], axis=0)

    def expert_step(accumulated, inputs):
        picks, gate_one, up_one, down_one = inputs
        owners = picks // TOPK
        chosen = padded_rows[owners]
        gate_part = jnp.dot(chosen, gate_one, preferred_element_type=jnp.float32)
        up_part = jnp.dot(chosen, up_one, preferred_element_type=jnp.float32)
        hidden = (jax.nn.silu(gate_part) * up_part).astype(jnp.bfloat16)
        result = jnp.dot(hidden, down_one, preferred_element_type=jnp.float32).astype(jnp.bfloat16)
        scaled = result.astype(jnp.float32) * padded_weights[picks][:, None]
        return (accumulated.at[owners].add(scaled, mode='drop'), None)
    routed, _ = lax.scan(expert_step, jnp.zeros((TOKENS, D), jnp.float32), (table, gate_weight, up_weight, down_weight))
    shared_hidden = (jax.nn.silu(jnp.dot(normed, shared_gate, preferred_element_type=jnp.float32)) * jnp.dot(normed, shared_up, preferred_element_type=jnp.float32)).astype(jnp.bfloat16)
    shared_term = jnp.dot(shared_hidden, shared_down, preferred_element_type=jnp.float32)
    return (routed + shared_term).astype(jnp.bfloat16)

def reference(queries, key_value, key_bias, out_weight, expert_input, norm_gain, routes, route_weights, gate_weight, up_weight, down_weight, shared_gate, shared_up, shared_down):
    mixer_output = mixer_reference(queries, key_value, key_bias, out_weight)
    expert_output = experts_reference(expert_input, norm_gain, routes, route_weights, gate_weight, up_weight, down_weight, shared_gate, shared_up, shared_down)
    return (mixer_output, expert_output)
```

```python
import functools

import jax
import jax.numpy as jnp
from jax import lax
from jax.experimental import pallas as pl
from jax.experimental.pallas import tpu as pltpu
from jax.sharding import PartitionSpec as P


def stick_kernel(place_ref, query_ref, own_ref, own_bias_ref, visit_ref, visit_bias_ref, out_ref, *, distances):
    span_rows, width = query_ref.shape
    head_dim = own_ref.shape[1] // 2
    heads = width // head_dim
    tile = min(128, span_rows)
    rows_of = lax.broadcasted_iota(jnp.int32, (span_rows, span_rows), 0)
    columns_of = lax.broadcasted_iota(jnp.int32, (span_rows, span_rows), 1)
    later = (rows_of > columns_of).astype(jnp.bfloat16)

    def piece(query, keys_values, bias, kept, allowed):
        keys = keys_values[:, :head_dim]
        values = keys_values[:, head_dim:]
        logits = lax.dot_general(
            query, keys, (((1,), (1,)), ((), ())), preferred_element_type=jnp.float32
        )
        logits = logits * 0.125 + bias.astype(jnp.float32)
        keep = -(jnp.maximum(logits, 0.0) + jnp.log(1.0 + jnp.exp(-jnp.abs(logits))))
        own_log = logits + keep
        if allowed is not None:
            keep = jnp.where(allowed, keep, 0.0)
        upper = keep.astype(jnp.bfloat16)
        lower = (keep - upper.astype(jnp.float32)).astype(jnp.bfloat16)
        after = jnp.dot(upper, later, preferred_element_type=jnp.float32) + jnp.dot(
            lower, later, preferred_element_type=jnp.float32
        )
        total = own_log + after
        if kept is not None:
            total = total + kept
        weights = jnp.exp(total)
        if allowed is not None:
            weights = jnp.where(allowed, weights, 0.0)
        update = jnp.dot(
            weights.astype(jnp.bfloat16), values, preferred_element_type=jnp.float32
        )
        return update, jnp.sum(keep, axis=1, keepdims=True)

    def one_tile(index, carry):
        start = pl.multiple_of(index * tile, tile)
        query_rows = query_ref[pl.ds(start, tile), :]
        position = start + lax.broadcasted_iota(jnp.int32, (tile, span_rows), 0)
        allowed = lax.broadcasted_iota(jnp.int32, (tile, span_rows), 1) < position
        totals, kept_sums = [], []
        for head in range(heads):
            query = query_rows[:, head * head_dim : (head + 1) * head_dim]
            total, kept = piece(query, own_ref[...], own_bias_ref[...], None, allowed)
            totals.append(total)
            kept_sums.append(kept)
        state = (tuple(totals), tuple(kept_sums))
        for distance in range(1, distances + 1):

            def include(earlier, distance=distance):
                totals, kept_sums = earlier
                new_totals, new_kept = [], []
                for head in range(heads):
                    query = query_rows[:, head * head_dim : (head + 1) * head_dim]
                    update, kept = piece(
                        query,
                        visit_ref[distance - 1],
                        visit_bias_ref[distance - 1],
                        kept_sums[head],
                        None,
                    )
                    new_totals.append(totals[head] + update)
                    new_kept.append(kept_sums[head] + kept)
                return (tuple(new_totals), tuple(new_kept))

            state = lax.cond(distance <= place_ref[0], include, lambda earlier: earlier, state)
        out_ref[pl.ds(start, tile), :] = jnp.concatenate(state[0], axis=1).astype(jnp.bfloat16)
        return carry

    lax.fori_loop(0, span_rows // tile, one_tile, 0)


def attended_heads(queries, key_value, key_bias):
    span_rows, key_groups, pair_width = key_value.shape
    head_dim = pair_width // 2
    group_width = queries.shape[1] // key_groups
    axis_size = lax.axis_size("ep")
    chain_length = axis_size // max(1, axis_size // 4)
    places = [min((i + 2) % chain_length, i) for i in range(axis_size)]
    distances = max(places)
    device_place = lax.axis_index("ep")
    chain_place = jnp.minimum((device_place + 2) % chain_length, device_place)
    packed = jnp.concatenate(
        [key_value.reshape(-1, pair_width), key_bias.reshape(-1, pair_width)], axis=0
    )
    own_rows = span_rows * key_groups
    visits, visit_biases = [], []
    for distance in range(1, distances + 1):
        route = [(i - distance, i) for i in range(axis_size) if places[i] >= distance]
        got = lax.ppermute(packed, "ep", route)
        visits.append(got[:own_rows].reshape(span_rows, key_groups, pair_width))
        visit_biases.append(got[own_rows:].reshape(key_groups, span_rows))
    if not visits:
        visits, visit_biases = [key_value], [key_bias]
    visits = jnp.stack(visits)
    visit_biases = jnp.stack(visit_biases)
    place = chain_place.astype(jnp.int32).reshape(1)
    memory = pl.BlockSpec(memory_space=pltpu.VMEM)
    outputs = []
    for group in range(key_groups):
        outputs.append(
            pl.pallas_call(
                functools.partial(stick_kernel, distances=distances),
                out_shape=jax.ShapeDtypeStruct((span_rows, group_width), jnp.bfloat16),
                in_specs=[pl.BlockSpec(memory_space=pltpu.SMEM)] + [memory] * 5,
                out_specs=memory,
                name="stick",
            )(
                place,
                queries[:, group * group_width : (group + 1) * group_width],
                key_value[:, group],
                key_bias[group : group + 1],
                visits[:, :, group],
                visit_biases[:, group : group + 1],
            )
        )
    return outputs[0] if key_groups == 1 else jnp.concatenate(outputs, axis=1)


def projected(attended, out_weight):
    return lax.psum_scatter(
        jnp.dot(attended, out_weight, preferred_element_type=jnp.float32).astype(jnp.bfloat16),
        "tp",
        scatter_dimension=0,
        tiled=True,
    )


def expert_rows(arrived, gate_weight, up_weight, down_weight):
    sources, capacity, model_width = arrived.shape
    flat_rows = arrived.reshape(sources * capacity, model_width)
    gate_part = jnp.dot(flat_rows, gate_weight[0], preferred_element_type=jnp.float32)
    up_part = jnp.dot(flat_rows, up_weight[0], preferred_element_type=jnp.float32)
    hidden = (jax.nn.silu(gate_part) * up_part).astype(jnp.bfloat16)
    result = jnp.dot(hidden, down_weight[0], preferred_element_type=jnp.float32).astype(
        jnp.bfloat16
    )
    return result.reshape(sources, capacity, model_width)


def experts_and_mixer(
    queries,
    key_value,
    key_bias,
    out_weight,
    expert_input,
    norm_gain,
    routes,
    route_weights,
    gate_weight,
    up_weight,
    down_weight,
    shared_gate,
    shared_up,
    shared_down,
):
    tokens, top_count = routes.shape
    model_width = expert_input.shape[1]
    experts = lax.axis_size("ep") * lax.axis_size("tp")
    capacity = max(2, 3 * tokens * top_count // (2 * experts))
    widened = expert_input.astype(jnp.float32)
    normed = (
        widened * lax.rsqrt(jnp.mean(widened * widened, axis=-1, keepdims=True) + 1e-06) * norm_gain
    ).astype(jnp.bfloat16)
    names = jnp.arange(experts, dtype=jnp.int32)
    named = routes.T[:, None, :] == names[None, :, None]
    chosen = jnp.any(named, axis=0)
    token_weight = jnp.sum(jnp.where(named, route_weights.T[:, None, :], 0.0), axis=0)
    order = jnp.arange(tokens, dtype=jnp.int32)
    earlier = (order[:, None] < order[None, :]).astype(jnp.bfloat16)
    slots = jnp.dot(chosen.astype(jnp.bfloat16), earlier, preferred_element_type=jnp.float32)
    slots = jnp.where(chosen, slots.astype(jnp.int32), -1)
    picked = slots[:, None, :] == jnp.arange(capacity, dtype=jnp.int32)[None, :, None]
    picker = picked.astype(jnp.bfloat16).reshape(experts * capacity, tokens)
    outgoing = jnp.dot(picker, normed, preferred_element_type=jnp.float32).astype(jnp.bfloat16)
    outgoing = outgoing.reshape(experts, capacity, model_width)
    arrived = lax.all_to_all(outgoing, ("ep", "tp"), split_axis=0, concat_axis=0, tiled=True)
    attended = attended_heads(queries, key_value, key_bias)
    arrived, attended = lax.optimization_barrier((arrived, attended))
    came_back = lax.all_to_all(
        expert_rows(arrived, gate_weight, up_weight, down_weight),
        ("ep", "tp"),
        split_axis=0,
        concat_axis=0,
        tiled=True,
    )
    mixer_output = projected(attended, out_weight)
    shared_hidden = (
        jax.nn.silu(jnp.dot(normed, shared_gate, preferred_element_type=jnp.float32))
        * jnp.dot(normed, shared_up, preferred_element_type=jnp.float32)
    ).astype(jnp.bfloat16)
    shared_term = jnp.dot(shared_hidden, shared_down, preferred_element_type=jnp.float32)
    upper = token_weight.astype(jnp.bfloat16)
    lower = (token_weight - upper.astype(jnp.float32)).astype(jnp.bfloat16)
    parts = jnp.stack([upper, lower], axis=1)
    mixing = jnp.where(picked[:, :, None, :], parts[:, None], jnp.zeros((), jnp.bfloat16))
    mixing = mixing.reshape(experts * capacity, 2 * tokens)
    back_rows = came_back.reshape(experts * capacity, model_width)
    routed = lax.dot_general(
        mixing, back_rows, (((0,), (0,)), ((), ())), preferred_element_type=jnp.float32
    )
    expert_output = (routed[:tokens] + routed[tokens:] + shared_term).astype(jnp.bfloat16)
    return (mixer_output, expert_output)


def solution(mesh):
    placed = (
        P(("grp", "ep"), "tp"),
        P(("grp", "ep"), "tp", None),
        P("tp", ("grp", "ep")),
        P("tp", None),
        P(("grp", "ep", "tp"), None),
        P(),
        P(("grp", "ep", "tp"), None),
        P(("grp", "ep", "tp"), None),
        P(("ep", "tp"), None, None),
        P(("ep", "tp"), None, None),
        P(("ep", "tp"), None, None),
        P(),
        P(),
        P(),
    )
    return jax.shard_map(
        experts_and_mixer,
        mesh=mesh,
        in_specs=placed,
        out_specs=(P(("grp", "ep", "tp"), None), P(("grp", "ep", "tp"), None)),
        check_vma=False,
    )
```
